32 devices in a mesh: sp: 8 (over z, x), tp: 4 (over y, core).
Axes of the slice: x: 2, y: 2, z: 4, core: 2. Of those that a mesh axis runs over, the one named last changes fastest.
Arguments:
- layer_source_vector: bfloat16 [2560, 2048], P('sp', 'tp'), may hold values from -40 to 40
- attention_lane_source: bfloat16 [2560, 1024], P('sp', 'tp'), may hold values from -6 to 6
- result_valve_logits: bfloat16 [2560, 1024], P('sp', 'tp'), may hold values from -6 to 6
- memory_write_matrix: bfloat16 [2560, 512], P('sp'), may hold values from -6 to 6
- memory_query_matrix: bfloat16 [2560, 512], P('sp'), may hold values from -6 to 6
- increment_logits: bfloat16 [2, 2560, 16], P(None, 'sp', 'tp'), may hold values from -3 to 3
- increment_offset: float32 [2, 16], P(None, 'tp'), may hold values from -16 to -3
- log_fade_speed: float32 [2, 16], P(None, 'tp'), may hold values from 0 to 1.4
- extra_log_fade: float32 [2, 2560, 16], P(None, 'sp', 'tp'), may hold values from -3 to 0
- attention_bypass_factor: float32 [16], P('tp'), may hold values from 0.1 to 1.9
- attention_lane_kernel: bfloat16 [5, 1024], P(None, 'tp'), may hold values from -2.5 to 2.5
- memory_write_kernel: bfloat16 [5, 512], replicated, may hold values from -2.5 to 2.5
- memory_query_kernel: bfloat16 [5, 512], replicated, may hold values from -2.5 to 2.5
- cluster_rescale_factor: float32 [1024], P('tp'), may hold values from 0.1 to 1.9
- blender_result_matrix: bfloat16 [1024, 2048], P(None, 'tp'), may hold values from -0.1875 to 0.1875
- specialist_rescale_factor: float32 [2048], P('tp'), may hold values from 0.1 to 1.9
- chosen_specialists: int32 [2560, 2], P('sp'), may hold values from 0 to 7, all different within a row; in each aligned block of 320 rows (0 to 319, 320 to 639, ...) at most 120 rows name the same one
- specialist_shares: float32 [2560, 2], P('sp'), may hold values from 0.25 to 1.25
- specialist_valve_matrix: bfloat16 [8, 2048, 2048], P('sp', None, 'tp'), may hold values from -0.125 to 0.125
- specialist_raising_matrix: bfloat16 [8, 2048, 2048], P('sp', None, 'tp'), may hold values from -0.125 to 0.125
- specialist_lowering_matrix: bfloat16 [8, 2048, 2048], P('sp', None, 'tp'), may hold values from -0.125 to 0.125
- common_valve_matrix: bfloat16 [2048, 2048], P(None, 'tp'), may hold values from -0.125 to 0.125
- common_raising_matrix: bfloat16 [2048, 2048], P(None, 'tp'), may hold values from -0.125 to 0.125
- common_lowering_matrix: bfloat16 [2048, 2048], P(None, 'tp'), may hold values from -0.125 to 0.125
Outputs:
- result: bfloat16 [2560, 2048], P('sp', 'tp')
The draws below stay inside these ranges and needn't reach their ends.
Inputs may be any that keep to these rules, and one draw needn't show every extreme that they name: `chosen_specialists`: each row names 2 different experts; among the rows of one index of sp no expert is named more than 120 times, a bound that some block reaches there.
All inputs are finite; a program needn't handle non-finite values.
Results may differ from the reference program's by a relative error of at most 0.013.
Values may be sent and summed in bfloat16 or wider, within the bound.
A program may use at most 64 MiB of HBM per device.

```python
import math
import jax
import jax.numpy as jnp
import numpy as np
from jax import lax

D = 2048
HEADS = 16
HEAD_DIM = 64
GROUPS = 4
STATE = 128
CONV = 5
EXP_FF = 2048
SH_FF = 2048
TOP = 2
TOK_DEV = 320
WIDTH = 1024
TOKENS = 2560
EXPERTS = 8
CAP = 120
N_SP = 8


def draw_layer_source_vector(key, part):
    first, second = jax.random.split(key, 2)
    ramp = jnp.exp(math.log(0.5) + math.log(4.0) * jnp.arange(D, dtype=jnp.float32) / (D - 1))
    columns = ramp * jnp.exp(jax.random.uniform(second, (D,), jnp.float32, -0.5, 0.5))
    base = jnp.clip(jax.random.normal(first, (TOKENS, D), jnp.float32), -4.0, 4.0)
    return (base * columns[None, :]).astype(jnp.bfloat16)


def draw_increment_logits(key, part):
    first, second = jax.random.split(key)
    blocks = TOKENS // TOK_DEV
    offset = jax.random.uniform(second, (2, blocks, 1, HEADS), jnp.float32, -0.7, 0.7)
    offset = jnp.broadcast_to(offset, (2, blocks, TOK_DEV, HEADS)).reshape(2, TOKENS, HEADS)
    noise = 0.5 * jnp.clip(jax.random.normal(first, (2, TOKENS, HEADS), jnp.float32), -4.0, 4.0)
    return (noise + offset).astype(jnp.bfloat16)


def draw_increment_offset(key, part):
    first, second, third = jax.random.split(key, 3)
    share = 0.5
    slow = jax.random.uniform(first, (2, HEADS), jnp.float32) < share
    slow_step = jax.random.uniform(second, (2, HEADS), jnp.float32, 0.1, 0.4) / TOKENS
    fast_step = jnp.exp(jax.random.uniform(third, (2, HEADS), jnp.float32, math.log(0.005), math.log(0.02)))
    return jnp.log(jnp.where(slow, slow_step, fast_step)).astype(jnp.float32)


def draw_extra_log_fade(key, part):
    first, second = jax.random.split(key)
    spots = jax.random.randint(first, (2, 4, HEADS), 0, TOKENS)
    strength = jnp.log(jax.random.uniform(second, (2, 4, HEADS), jnp.float32, 0.5, 0.8))
    hits = jnp.arange(TOKENS)[None, None, :, None] == spots[:, :, None, :]
    return jnp.sum(jnp.where(hits, strength[:, :, None, :], 0.0), axis=1).astype(jnp.float32)


def level_of(own_key, extent, shards, low, top_value):
    def one(dim, shards_of):
        steps = jax.random.uniform(jax.random.fold_in(jax.random.fold_in(own_key, 6), dim), (shards_of,), jnp.float32, low / len(shards), top_value / len(shards))
        return jnp.repeat(jnp.exp(steps), extent[dim] // shards_of).reshape((-1,) + (1,) * (len(extent) - dim - 1))

    level = one(*shards[0])
    for cut in shards[1:]:
        level = level * one(*cut)
    return level


def assign_block(rng, own, number, rows, amount, top, limit, lean):
    order = jax.random.permutation(rng, amount)
    packed, common = load_shares(amount, rows * top, limit, lean, True), load_shares(amount, rows * top, limit, lean, False)
    places = jnp.arange(amount)

    def named(lengths, offset_by):
        used = int((lengths > 0).sum())
        fixed = max(1, used // 4)
        passed = fixed + (places - fixed + offset_by * (used - fixed)) % max(1, amount - fixed)
        return jnp.zeros((amount,), jnp.int32).at[order[jnp.where(places < fixed, places, passed)]].set(jnp.asarray(lengths, jnp.int32))

    lengths = jnp.where(number % 4 == 0, named(packed, number // 4), named(common, number - number // 4 - 1))
    mixed = jax.random.permutation(jax.random.fold_in(own, 3), amount)
    source_of, receiver = mixed[0:amount // 2 * 2:2], mixed[1:amount // 2 * 2:2]
    slack = jnp.minimum(lengths[source_of] - 1, limit - lengths[receiver]) // 2
    slack = jnp.where((source_of == order[0]) | (receiver == order[0]) | (lengths[receiver] == 0), 0, jnp.maximum(slack, 0))
    passed = jax.random.randint(jax.random.fold_in(own, 4), (amount // 2,), 0, 1 << 20) % (slack + 1)
    lengths = lengths.at[source_of].add(-passed).at[receiver].add(passed)
    labels = jnp.searchsorted(jnp.cumsum(lengths), jnp.arange(rows * top), side="right").astype(jnp.int32)
    listing = labels.reshape(top, rows).T
    listing = listing[jax.random.permutation(jax.random.fold_in(own, 1), rows)]
    offset_by = jax.random.randint(jax.random.fold_in(own, 2), (rows, 1), 0, top)
    return jnp.take_along_axis(listing, (jnp.arange(top)[None, :] + offset_by) % top, axis=1)


def load_shares(amount, total, reach, skew, full):
    portions = [(1 << 20) // math.isqrt(grade ** skew) + 1 for grade in range(1, amount + 1)]
    largest = reach if full else min(reach, max(-(-total // amount), total * portions[0] // sum(portions)))
    least = 1 if total - largest >= amount - 1 else 0
    holding, rest = [largest] + [least] * (amount - 1), total - largest - least * (amount - 1)
    while rest > 0:
        movable = [i for i in range(1, amount) if holding[i] < largest] or [i for i in range(1, amount) if holding[i] < reach]
        mass, budget = sum([portions[i] for i in movable]), rest
        for i in movable:
            extra = min(reach - holding[i], max(1, budget * portions[i] // mass), rest)
            holding[i] = holding[i] + extra
            rest = rest - extra
    return np.array(holding)


def centred(stream_key, dims, width, reach, cuts=(), kind=jnp.bfloat16):
    entries = width * jax.random.normal(stream_key, dims, jnp.float32)
    if cuts:
        entries = entries * level_of(stream_key, dims, cuts, -0.22, 0.18)
    return jnp.clip(entries, -reach, reach).astype(kind)


def setup_inputs(seed: int = 0) -> dict:
    seeds = jax.random.split(jax.random.key(seed), 25)
    layer_source_vector = draw_layer_source_vector(jax.random.fold_in(seeds[24], 71), 0)
    attention_lane_source = centred(seeds[1], (TOKENS, WIDTH), 1.0, 6.0, ((0, 8), (1, 4)))
    result_valve_logits = centred(seeds[2], (TOKENS, WIDTH), 1.0, 6.0, ((0, 8), (1, 4)))
    memory_write_matrix = centred(seeds[3], (TOKENS, GROUPS * STATE), 1.0, 6.0, ((0, 8),))
    memory_query_matrix = centred(seeds[4], (TOKENS, GROUPS * STATE), 1.0, 6.0, ((0, 8),))
    increment_logits = draw_increment_logits(jax.random.fold_in(seeds[24], 71), 0)
    increment_offset = draw_increment_offset(jax.random.fold_in(seeds[24], 71), 0)
    log_fade_speed = jnp.clip(1.4 * jax.random.uniform(seeds[7], (2, HEADS), jnp.float32) ** level_of(seeds[7], (2, HEADS), ((1, 4),), -0.2, 0.2), 0.0, 1.4)
    extra_log_fade = draw_extra_log_fade(jax.random.fold_in(seeds[24], 71), 0)
    attention_bypass_factor = jnp.clip(1.0 + 0.18 * jax.random.normal(seeds[9], (HEADS,), jnp.float32), 0.1, 1.9)
    attention_lane_kernel = centred(seeds[10], (CONV, WIDTH), CONV ** -0.5, 2.5, ((1, 4),))
    memory_write_kernel = centred(seeds[11], (CONV, GROUPS * STATE), CONV ** -0.5, 2.5)
    memory_query_kernel = centred(seeds[12], (CONV, GROUPS * STATE), CONV ** -0.5, 2.5)
    cluster_rescale_factor = jnp.clip(1.0 + 0.18 * jax.random.normal(seeds[13], (WIDTH,), jnp.float32), 0.1, 1.9)
    blender_result_matrix = centred(seeds[14], (WIDTH, D), WIDTH ** -0.5, 0.1875, ((1, 4),))
    specialist_rescale_factor = jnp.clip(1.0 + 0.18 * jax.random.normal(seeds[15], (D,), jnp.float32), 0.1, 1.9)
    chosen_specialists_keys = jax.random.split(jax.random.fold_in(seeds[16], 1), TOKENS // TOK_DEV)
    chosen_specialists_turns = jax.random.permutation(jax.random.fold_in(seeds[16], 3), TOKENS // TOK_DEV)
    chosen_specialists = jax.vmap(lambda own, number: assign_block(jax.random.fold_in(seeds[16], 2), own, number, TOK_DEV, EXPERTS, TOP, CAP, 1))(chosen_specialists_keys, chosen_specialists_turns).reshape((TOKENS, TOP))
    specialist_shares = jnp.clip(0.25 + 1.0 * jax.random.uniform(seeds[17], (TOKENS, TOP), jnp.float32) ** level_of(seeds[17], (TOKENS, TOP), ((0, 8),), -0.2, 0.2), 0.25, 1.25)
    specialist_valve_matrix = centred(seeds[18], (EXPERTS, D, EXP_FF), D ** -0.5, 0.125, ((0, 8), (2, 4)))
    specialist_raising_matrix = centred(seeds[19], (EXPERTS, D, EXP_FF), D ** -0.5, 0.125, ((0, 8), (2, 4)))
    specialist_lowering_matrix = centred(seeds[20], (EXPERTS, EXP_FF, D), EXP_FF ** -0.5, 0.125, ((0, 8), (2, 4)))
    common_valve_matrix = centred(seeds[21], (D, SH_FF), D ** -0.5, 0.125, ((1, 4),))
    common_raising_matrix = centred(seeds[22], (D, SH_FF), D ** -0.5, 0.125, ((1, 4),))
    common_lowering_matrix = centred(seeds[23], (SH_FF, D), SH_FF ** -0.5, 0.125, ((1, 4),))
    return dict(layer_source_vector=layer_source_vector, attention_lane_source=attention_lane_source, result_valve_logits=result_valve_logits, memory_write_matrix=memory_write_matrix, memory_query_matrix=memory_query_matrix, increment_logits=increment_logits, increment_offset=increment_offset, log_fade_speed=log_fade_speed, extra_log_fade=extra_log_fade, attention_bypass_factor=attention_bypass_factor, attention_lane_kernel=attention_lane_kernel, memory_write_kernel=memory_write_kernel, memory_query_kernel=memory_query_kernel, cluster_rescale_factor=cluster_rescale_factor, blender_result_matrix=blender_result_matrix, specialist_rescale_factor=specialist_rescale_factor, chosen_specialists=chosen_specialists, specialist_shares=specialist_shares, specialist_valve_matrix=specialist_valve_matrix, specialist_raising_matrix=specialist_raising_matrix, specialist_lowering_matrix=specialist_lowering_matrix, common_valve_matrix=common_valve_matrix, common_raising_matrix=common_raising_matrix, common_lowering_matrix=common_lowering_matrix)


def conv_silu(values, taps):
    half = CONV // 2
    length = values.shape[0]
    padded = jnp.pad(values, ((half, half), (0, 0)))
    total = jnp.zeros(values.shape, jnp.float32)
    for offset in range(CONV):
        total = total + padded[offset:offset + length].astype(jnp.float32) * taps[offset].astype(jnp.float32)
    return jax.nn.silu(total).astype(jnp.bfloat16)

def combine_states(earlier, later):
    return (earlier[0] + later[0], jnp.exp(later[0])[:, None, None] * earlier[1] + later[1])

def block_parts(inputs):
    x_block, b_block, c_block, step_block, log_block = inputs
    spread = HEADS // GROUPS
    scores = jnp.einsum('tgn,sgn->gts', c_block.astype(jnp.float32), b_block.astype(jnp.float32), precision=lax.Precision.HIGHEST)
    scores = jnp.repeat(scores, spread, axis=0)
    forward_cum = jnp.cumsum(log_block[0], axis=0)
    backward_cum = jnp.cumsum(log_block[1], axis=0) - log_block[1]
    forward_total = forward_cum[-1]
    backward_total = backward_cum[-1] + log_block[1][-1]
    length = x_block.shape[0]
    position = jnp.arange(length)
    lower = position[:, None] >= position[None, :]
    upper = position[:, None] <= position[None, :]
    forward_gap = forward_cum.T[:, :, None] - forward_cum.T[:, None, :]
    backward_gap = backward_cum.T[:, None, :] - backward_cum.T[:, :, None]
    forward_part = jnp.where(lower, jnp.exp(jnp.where(lower, forward_gap, 0.0)), 0.0) * step_block[0].T[:, None, :]
    backward_part = jnp.where(upper, jnp.exp(jnp.where(upper, backward_gap, 0.0)), 0.0) * step_block[1].T[:, None, :]
    mixing = (scores * (forward_part + backward_part)).astype(jnp.bfloat16)
    inner = jnp.einsum('hts,shp->thp', mixing.astype(jnp.float32), x_block.astype(jnp.float32), precision=lax.Precision.HIGHEST)
    forward_scale = jnp.exp(forward_total[None, :] - forward_cum) * step_block[0]
    backward_scale = jnp.exp(backward_cum) * step_block[1]
    scaled = (jnp.stack([forward_scale, backward_scale])[..., None] * x_block.astype(jnp.float32)[None]).astype(jnp.bfloat16)
    b_heads = jnp.repeat(b_block, spread, axis=1)
    states = jnp.einsum('dshp,shn->dhpn', scaled.astype(jnp.float32), b_heads.astype(jnp.float32), precision=lax.Precision.HIGHEST)
    logs = jnp.stack([forward_total, backward_total])
    return (inner, states, logs)

def run_expert(item):
    rows_in, gate_w, up_w, down_w = item
    hidden = (jax.nn.silu(jnp.dot(rows_in, gate_w, preferred_element_type=jnp.float32)) * jnp.dot(rows_in, up_w, preferred_element_type=jnp.float32)).astype(jnp.bfloat16)
    return jnp.dot(hidden, down_w, preferred_element_type=jnp.float32).astype(jnp.bfloat16)

def reference(layer_source_vector, attention_lane_source, result_valve_logits, memory_write_matrix, memory_query_matrix, increment_logits, increment_offset, log_fade_speed, extra_log_fade, attention_bypass_factor, attention_lane_kernel, memory_write_kernel, memory_query_kernel, cluster_rescale_factor, blender_result_matrix, specialist_rescale_factor, chosen_specialists, specialist_shares, specialist_valve_matrix, specialist_raising_matrix, specialist_lowering_matrix, common_valve_matrix, common_raising_matrix, common_lowering_matrix):
    x_conv = conv_silu(attention_lane_source, attention_lane_kernel)
    b_conv = conv_silu(memory_write_matrix, memory_write_kernel)
    c_conv = conv_silu(memory_query_matrix, memory_query_kernel)
    increment_lengths = jax.nn.softplus(increment_logits.astype(jnp.float32) + increment_offset[:, None, :])
    log_fade_amount = -jnp.exp(log_fade_speed)[:, None, :] * increment_lengths + extra_log_fade
    blocks = N_SP
    x_blocks = x_conv.reshape(blocks, TOK_DEV, HEADS, HEAD_DIM)
    b_blocks = b_conv.reshape(blocks, TOK_DEV, GROUPS, STATE)
    c_blocks = c_conv.reshape(blocks, TOK_DEV, GROUPS, STATE)
    step_blocks = increment_lengths.reshape(2, blocks, TOK_DEV, HEADS).transpose(1, 0, 2, 3)
    log_blocks = log_fade_amount.reshape(2, blocks, TOK_DEV, HEADS).transpose(1, 0, 2, 3)
    inner, states, logs = lax.map(block_parts, (x_blocks, b_blocks, c_blocks, step_blocks, log_blocks))

    def chain_step(carry, item):
        return (combine_states(carry, item), carry)
    zero = (jnp.zeros((HEADS,), jnp.float32), jnp.zeros((HEADS, HEAD_DIM, STATE), jnp.float32))
    _, carried_forward = lax.scan(chain_step, zero, (logs[:, 0], states[:, 0]))
    _, carried_backward = lax.scan(chain_step, zero, (logs[:, 1], states[:, 1]), reverse=True)
    carried = jnp.stack([carried_forward[1], carried_backward[1]], axis=1).astype(jnp.bfloat16)
    c_heads = jnp.repeat(c_blocks, HEADS // GROUPS, axis=2)
    readout = jnp.einsum('kthn,kdhpn->kdthp', c_heads.astype(jnp.float32), carried.astype(jnp.float32), precision=lax.Precision.HIGHEST)
    forward_cum = jnp.cumsum(log_blocks[:, 0], axis=1)
    backward_cum = jnp.cumsum(log_blocks[:, 1], axis=1) - log_blocks[:, 1]
    backward_total = backward_cum[:, -1] + log_blocks[:, 1, -1]
    mixer = inner + jnp.exp(forward_cum)[..., None] * readout[:, 0] + jnp.exp(backward_total[:, None] - backward_cum)[..., None] * readout[:, 1] + attention_bypass_factor[None, None, :, None] * x_blocks.astype(jnp.float32)
    mixer = mixer.reshape(TOKENS, HEADS, HEAD_DIM)
    gated = mixer * jax.nn.silu(result_valve_logits.astype(jnp.float32)).reshape(TOKENS, HEADS, HEAD_DIM)
    grouped = gated.reshape(TOKENS, GROUPS, -1)
    scale = lax.rsqrt(lax.optimization_barrier(jnp.mean(grouped * grouped, axis=-1, keepdims=True)) + 1e-06)
    normed = ((grouped * scale).reshape(TOKENS, WIDTH) * cluster_rescale_factor[None, :]).astype(jnp.bfloat16)
    after_mixer = (layer_source_vector.astype(jnp.float32) + jnp.dot(normed, blender_result_matrix, preferred_element_type=jnp.float32)).astype(jnp.bfloat16)
    resid = after_mixer.astype(jnp.float32)
    features = (resid * lax.rsqrt(lax.optimization_barrier(jnp.mean(resid * resid, axis=1, keepdims=True)) + 1e-06) * specialist_rescale_factor[None, :]).astype(jnp.bfloat16)
    shared_hidden = (jax.nn.silu(jnp.dot(features, common_valve_matrix, preferred_element_type=jnp.float32)) * jnp.dot(features, common_raising_matrix, preferred_element_type=jnp.float32)).astype(jnp.bfloat16)
    shared_out = jnp.dot(shared_hidden, common_lowering_matrix, preferred_element_type=jnp.float32).astype(jnp.bfloat16)
    flat = chosen_specialists.reshape(blocks, TOK_DEV * TOP)
    one_hot = (flat[..., None] == jnp.arange(EXPERTS, dtype=jnp.int32)[None, None, :]).astype(jnp.int32)
    rank = lax.optimization_barrier(jnp.sum((jnp.cumsum(one_hot, axis=1) - one_hot) * one_hot, axis=2))
    place = (jnp.arange(blocks, dtype=jnp.int32)[:, None] * CAP + rank).reshape(-1).astype(jnp.int32)
    expert_flat = flat.reshape(-1).astype(jnp.int32)
    token = (jnp.arange(TOKENS * TOP) // TOP).astype(jnp.int32)
    buffer = jnp.zeros((EXPERTS, blocks * CAP, D), jnp.bfloat16).at[expert_flat, place].set(features[token])
    outputs = lax.map(run_expert, (buffer, specialist_valve_matrix, specialist_raising_matrix, specialist_lowering_matrix))
    picked = outputs[expert_flat, place].astype(jnp.float32).reshape(TOKENS, TOP, D)
    routed = lax.optimization_barrier(jnp.sum(picked * specialist_shares[:, :, None], axis=1))
    return (resid + shared_out.astype(jnp.float32) + routed).astype(jnp.bfloat16)
```

```python
import functools

import jax
import jax.numpy as jnp
from jax import lax
from jax.experimental import pallas as pl
from jax.experimental.pallas import tpu as pltpu
from jax.sharding import PartitionSpec as P

MESH = pl.DeviceIdType.MESH
KERNEL_DEVICES = 32

D = 2048
HEADS = 16
HEAD_DIM = 64
GROUPS = 4
STATE = 128
CONV = 5


def extended(cells, sides, width):
    for axis, dim in sides:
        count = lax.axis_size(axis)
        ends = count - 1
        head = lax.slice_in_dim(cells, 0, width, axis=dim)
        tail = lax.slice_in_dim(cells, cells.shape[dim] - width, cells.shape[dim], axis=dim)
        cells = jnp.concatenate(
            [
                lax.ppermute(tail, axis, [(i, (i + 1) % count) for i in range(ends)]),
                cells,
                lax.ppermute(head, axis, [((i + 1) % count, i) for i in range(ends)]),
            ],
            axis=dim,
        )
    return cells


def small_mesh():
    return lax.axis_size("sp") * lax.axis_size("tp") <= KERNEL_DEVICES


def greet(axis, peers):
    barrier = pltpu.get_barrier_semaphore()
    for a, peer in zip(axis, peers):
        pl.semaphore_signal(barrier, inc=1, device_id={a: peer}, device_id_type=MESH)
    pl.semaphore_wait(barrier, len(peers))


def remote(src, dst, send, recv, axis, peer):
    return pltpu.make_async_remote_copy(
        src_ref=src,
        dst_ref=dst,
        send_sem=send,
        recv_sem=recv,
        device_id={axis: peer},
        device_id_type=MESH,
    )


def gather_kernel(n, counts, *refs):
    m = len(counts)
    ins, outs = refs[:m], refs[m : 2 * m]
    send_sem, recv_sem, local_sem = refs[2 * m :]
    half = n // 2
    me = lax.axis_index("tp")
    row, core = me // 2, me % 2
    sibling = row * 2 + 1 - core
    onward = [((row + k) % half) * 2 + core for k in range(1, half)]
    origin = [((row + half - k) % half) * 2 + core for k in range(1, half)]
    theirs = [((row + half - k) % half) * 2 + 1 - core for k in range(1, half)]
    greet(["tp"] * half, [sibling] + onward)
    pieces = []
    for i, count in enumerate(counts):
        size = ins[i].shape[0] // count
        for c in range(count):
            pieces.append((i, c * size, size))

    def spot(i, start, size, who):
        width = ins[i].shape[1]
        return outs[i].at[
            pl.ds(start, size), pl.ds(pl.multiple_of(who * width, 128), width)
        ]

    started = []
    for p, (i, start, size) in enumerate(pieces):
        src = ins[i].at[pl.ds(start, size)]
        for k in range(half - 1):
            cp = remote(
                src, spot(i, start, size, me), send_sem.at[1 + k, p], recv_sem.at[1 + k, p], "tp", onward[k]
            )
            cp.start()
            started.append(cp)
    for p, (i, start, size) in enumerate(pieces):
        src = ins[i].at[pl.ds(start, size)]
        cp = remote(src, spot(i, start, size, me), send_sem.at[0, p], recv_sem.at[0, p], "tp", sibling)
        cp.start()
        started.append(cp)
    locals_ = []
    for i in range(m):
        cp = pltpu.make_async_copy(ins[i], spot(i, 0, ins[i].shape[0], me), local_sem.at[i])
        cp.start()
        locals_.append(cp)
    for p, (i, start, size) in enumerate(pieces):
        for k in range(half - 1):
            here = spot(i, start, size, origin[k])
            remote(here, here, send_sem.at[1 + k, p], recv_sem.at[1 + k, p], "tp", sibling).wait_recv()
            cp = remote(here, here, send_sem.at[half + k, p], recv_sem.at[half + k, p], "tp", sibling)
            cp.start()
            started.append(cp)
    for p, (i, start, size) in enumerate(pieces):
        here = spot(i, start, size, sibling)
        remote(here, here, send_sem.at[0, p], recv_sem.at[0, p], "tp", sibling).wait_recv()
        for k in range(half - 1):
            here = spot(i, start, size, theirs[k])
            remote(here, here, send_sem.at[half + k, p], recv_sem.at[half + k, p], "tp", sibling).wait_recv()
    for cp in started:
        cp.wait_send()
    for cp in locals_:
        cp.wait()


def gather_tp(arrays, counts, ident):
    n = lax.axis_size("tp")
    if not small_mesh():
        return [lax.all_gather(a, "tp", axis=1, tiled=True) for a in arrays]
    total = sum(counts)
    return pl.pallas_call(
        functools.partial(gather_kernel, n, counts),
        out_shape=[jax.ShapeDtypeStruct((a.shape[0], a.shape[1] * n), a.dtype) for a in arrays],
        in_specs=[pl.BlockSpec(memory_space=pltpu.VMEM)] * len(arrays),
        out_specs=[pl.BlockSpec(memory_space=pl.ANY)] * len(arrays),
        scratch_shapes=[
            pltpu.SemaphoreType.DMA((n, total)),
            pltpu.SemaphoreType.DMA((n, total)),
            pltpu.SemaphoreType.DMA((len(arrays),)),
        ],
        compiler_params=pltpu.CompilerParams(collective_id=ident, has_side_effects=True),
        name="gather_tp_%d" % ident,
    )(*arrays)


def swap_kernel(n, select, m, *refs):
    ins, outs = refs[:m], refs[m : 2 * m]
    send_sem, recv_sem, local_sem = refs[2 * m :]
    me = lax.axis_index("sp")
    peers = [(me + k) % n for k in range(1, n)]
    greet(["sp"] * (n - 1), peers)
    started = []
    for k in sorted(range(1, n), key=lambda v: -min(v, n - v)):
        for i in range(m):
            row = (me + k) // n if select else peers[k - 1]
            cp = remote(
                ins[i].at[row], outs[i].at[me], send_sem.at[i, k], recv_sem.at[i, k], "sp", peers[k - 1]
            )
            cp.start()
            started.append(cp)
    locals_ = []
    for i in range(m):
        cp = pltpu.make_async_copy(ins[i].at[0 if select else me], outs[i].at[me], local_sem.at[i])
        cp.start()
        locals_.append(cp)
    for k in range(1, n):
        for i in range(m):
            here = outs[i].at[(me + n - k) % n]
            remote(here, here, send_sem.at[i, k], recv_sem.at[i, k], "sp", peers[k - 1]).wait_recv()
    for cp in started:
        cp.wait_send()
    for cp in locals_:
        cp.wait()


def swap_sp(arrays, ident, select=False):
    n = lax.axis_size("sp")
    if not small_mesh():
        if select:
            later = jnp.arange(n) > lax.axis_index("sp")
            arrays = [
                jnp.where(later[:, None, None], a[0][None], a[1][None]) for a in arrays
            ]
        return [lax.all_to_all(a, "sp", split_axis=0, concat_axis=0, tiled=True) for a in arrays]
    m = len(arrays)
    return pl.pallas_call(
        functools.partial(swap_kernel, n, select, m),
        out_shape=[jax.ShapeDtypeStruct((n,) + a.shape[1:], a.dtype) for a in arrays],
        in_specs=[pl.BlockSpec(memory_space=pltpu.VMEM)] * m,
        out_specs=[pl.BlockSpec(memory_space=pl.ANY)] * m,
        scratch_shapes=[
            pltpu.SemaphoreType.DMA((m, n)),
            pltpu.SemaphoreType.DMA((m, n)),
            pltpu.SemaphoreType.DMA((m,)),
        ],
        compiler_params=pltpu.CompilerParams(collective_id=ident, has_side_effects=True),
        name="swap_sp_%d" % ident,
    )(*arrays)


def dispatch_kernel(n, t, in_ref, out_ref, go_s, go_r, fan_s, fan_r, local_sem):
    half = t // 2
    width = in_ref.shape[2]
    me, mine = lax.axis_index("sp"), lax.axis_index("tp")
    row, core = mine // 2, mine % 2
    sibling = row * 2 + 1 - core
    onward = [((row + k) % half) * 2 + core for k in range(1, half)]
    origin = [((row + half - k) % half) * 2 + core for k in range(1, half)]
    theirs = [((row + half - k) % half) * 2 + 1 - core for k in range(1, half)]
    peers = [(me + k) % n for k in range(1, n)]
    greet(["sp"] * (n - 1) + ["tp"] * half, peers + [sibling] + onward)

    def spot(source, who):
        return out_ref.at[source, :, pl.ds(pl.multiple_of(who * width, 128), width)]

    started = []
    for k in sorted(range(1, n), key=lambda v: -min(v, n - v)):
        cp = remote(in_ref.at[peers[k - 1]], spot(me, mine), go_s.at[k], go_r.at[k], "sp", peers[k - 1])
        cp.start()
        started.append(cp)
    keep = pltpu.make_async_copy(in_ref.at[me], spot(me, mine), local_sem.at[0])
    keep.start()

    def fan(k, src, source):
        for j in range(half - 1):
            cp = remote(src, spot(source, mine), fan_s.at[1 + j, k], fan_r.at[1 + j, k], "tp", onward[j])
            cp.start()
            started.append(cp)
        cp = remote(src, spot(source, mine), fan_s.at[0, k], fan_r.at[0, k], "tp", sibling)
        cp.start()
        started.append(cp)

    def hand(k, source):
        for j in range(half - 1):
            here = spot(source, origin[j])
            remote(here, here, fan_s.at[1 + j, k], fan_r.at[1 + j, k], "tp", sibling).wait_recv()
            cp = remote(here, here, fan_s.at[half + j, k], fan_r.at[half + j, k], "tp", sibling)
            cp.start()
            started.append(cp)

    fan(0, in_ref.at[me], me)
    order = [0] + sorted(range(1, n), key=lambda v: (min(v, n - v), v))
    source = [(me + n - k) % n for k in range(n)]
    for at, k in enumerate(order):
        if k:
            here = spot(source[k], mine)
            remote(here, here, go_s.at[k], go_r.at[k], "sp", peers[k - 1]).wait_recv()
            fan(k, here, source[k])
        if at >= 2:
            hand(order[at - 2], source[order[at - 2]])
    for k in order[-2:]:
        hand(k, source[k])
    for k in order:
        here = spot(source[k], sibling)
        remote(here, here, fan_s.at[0, k], fan_r.at[0, k], "tp", sibling).wait_recv()
        for j in range(half - 1):
            here = spot(source[k], theirs[j])
            remote(here, here, fan_s.at[half + j, k], fan_r.at[half + j, k], "tp", sibling).wait_recv()
    for cp in started:
        cp.wait_send()
    keep.wait()


def dispatch(outgoing, ident):
    n, t = lax.axis_size("sp"), lax.axis_size("tp")
    if not small_mesh():
        arrived = lax.all_to_all(outgoing, "sp", split_axis=0, concat_axis=0, tiled=True)
        return lax.all_gather(arrived, "tp", axis=2, tiled=True)
    return pl.pallas_call(
        functools.partial(dispatch_kernel, n, t),
        out_shape=jax.ShapeDtypeStruct(
            outgoing.shape[:2] + (outgoing.shape[2] * t,), outgoing.dtype
        ),
        in_specs=[pl.BlockSpec(memory_space=pltpu.VMEM)],
        out_specs=pl.BlockSpec(memory_space=pl.ANY),
        scratch_shapes=[
            pltpu.SemaphoreType.DMA((n,)),
            pltpu.SemaphoreType.DMA((n,)),
            pltpu.SemaphoreType.DMA((t, n)),
            pltpu.SemaphoreType.DMA((t, n)),
            pltpu.SemaphoreType.DMA((1,)),
        ],
        compiler_params=pltpu.CompilerParams(collective_id=ident, has_side_effects=True),
        name="dispatch_%d" % ident,
    )(outgoing)


def shards(
    layer_source_vector,
    attention_lane_source,
    result_valve_logits,
    memory_write_matrix,
    memory_query_matrix,
    increment_logits,
    increment_offset,
    log_fade_speed,
    extra_log_fade,
    attention_bypass_factor,
    attention_lane_kernel,
    memory_write_kernel,
    memory_query_kernel,
    cluster_rescale_factor,
    blender_result_matrix,
    specialist_rescale_factor,
    chosen_specialists,
    specialist_shares,
    specialist_valve_matrix,
    specialist_raising_matrix,
    specialist_lowering_matrix,
    common_valve_matrix,
    common_raising_matrix,
    common_lowering_matrix,
):
    length = attention_lane_source.shape[0]
    heads_here = increment_offset.shape[1]
    channels = attention_lane_source.shape[1]
    head_size = channels // heads_here
    spread = HEADS // GROUPS
    group = lax.axis_index("tp") * heads_here // spread
    b_own = lax.dynamic_slice_in_dim(memory_write_matrix, group * STATE, STATE, 1)
    c_own = lax.dynamic_slice_in_dim(memory_query_matrix, group * STATE, STATE, 1)
    joined = jnp.concatenate([attention_lane_source, b_own, c_own], axis=1)
    taps = jnp.concatenate(
        [
            attention_lane_kernel,
            lax.dynamic_slice_in_dim(memory_write_kernel, group * STATE, STATE, 1),
            lax.dynamic_slice_in_dim(memory_query_kernel, group * STATE, STATE, 1),
        ],
        axis=1,
    )
    padded = extended(joined, (("sp", 0),), CONV // 2)
    total = jnp.zeros(joined.shape, jnp.float32)
    for offset in range(CONV):
        total = total + padded[offset : offset + length].astype(jnp.float32) * taps[offset].astype(
            jnp.float32
        )
    convolved = jax.nn.silu(total).astype(jnp.bfloat16)
    x_conv = convolved[:, :channels].reshape(length, heads_here, head_size)
    b_conv = convolved[:, channels : channels + STATE]
    c_conv = convolved[:, channels + STATE :]
    increment_lengths = jax.nn.softplus(
        increment_logits.astype(jnp.float32) + increment_offset[:, None, :]
    )
    log_fade_amount = -jnp.exp(log_fade_speed)[:, None, :] * increment_lengths + extra_log_fade
    position = jnp.arange(length)
    lower = position[:, None] >= position[None, :]
    upper = position[:, None] <= position[None, :]
    both = jnp.concatenate([log_fade_amount[0], log_fade_amount[1]], axis=1)
    sums = jnp.dot(
        lower.astype(jnp.float32),
        both,
        precision=lax.Precision.HIGHEST,
        preferred_element_type=jnp.float32,
    )
    forward_cum = sums[:, :heads_here]
    backward_cum = sums[:, heads_here:] - log_fade_amount[1]
    forward_total = sums[-1, :heads_here]
    backward_total = sums[-1, heads_here:]
    scores = lax.dot_general(
        c_conv, b_conv, (((1,), (1,)), ((), ())), preferred_element_type=jnp.float32
    )
    forward_gap = forward_cum.T[:, :, None] - forward_cum.T[:, None, :]
    backward_gap = backward_cum.T[:, None, :] - backward_cum.T[:, :, None]
    forward_part = (
        jnp.where(lower, jnp.exp(jnp.where(lower, forward_gap, 0.0)), 0.0)
        * increment_lengths[0].T[:, None, :]
    )
    backward_part = (
        jnp.where(upper, jnp.exp(jnp.where(upper, backward_gap, 0.0)), 0.0)
        * increment_lengths[1].T[:, None, :]
    )
    mixing = (scores[None] * (forward_part + backward_part)).astype(jnp.bfloat16)
    inner = jnp.einsum("hts,shp->thp", mixing, x_conv, preferred_element_type=jnp.float32)
    forward_scale = jnp.exp(forward_total[None, :] - forward_cum) * increment_lengths[0]
    backward_scale = jnp.exp(backward_cum) * increment_lengths[1]
    scaled = (
        jnp.stack([forward_scale, backward_scale])[..., None] * x_conv.astype(jnp.float32)[None]
    ).astype(jnp.bfloat16)
    own_states = jnp.einsum("dshp,sn->dhpn", scaled, b_conv, preferred_element_type=jnp.float32)
    own_logs = jnp.stack([forward_total, backward_total])
    blocks = lax.axis_size("sp")
    own_index = lax.axis_index("sp")
    states_all, logs_all = swap_sp(
        [
            own_states.astype(jnp.bfloat16).reshape(2, heads_here * head_size, STATE),
            jnp.broadcast_to(own_logs[:, :, None], (2, heads_here, 128)),
        ],
        1,
        True,
    )
    logs_all = logs_all[:, :, 0]
    states_all = states_all.reshape(blocks, heads_here, head_size, STATE).astype(jnp.float32)
    index = jnp.arange(blocks)
    earlier = (index < own_index)[:, None]
    later = (index > own_index)[:, None]
    after = (index[None, :] > index[:, None])[:, :, None]
    ahead = (index[None, :] < index[:, None])[:, :, None]
    gap_forward = jnp.sum(jnp.where(after & earlier[None], logs_all[None], 0.0), axis=1)
    gap_backward = jnp.sum(jnp.where(ahead & later[None], logs_all[None], 0.0), axis=1)
    weight_forward = jnp.where(earlier, jnp.exp(jnp.where(earlier, gap_forward, 0.0)), 0.0)
    weight_backward = jnp.where(later, jnp.exp(jnp.where(later, gap_backward, 0.0)), 0.0)
    weights = jnp.stack([weight_forward, weight_backward])
    carried = jnp.sum(weights[:, :, :, None, None] * states_all[None], axis=1).astype(jnp.bfloat16)
    readout = jnp.einsum("tn,dhpn->dthp", c_conv, carried, preferred_element_type=jnp.float32)
    mixer = (
        inner
        + jnp.exp(forward_cum)[..., None] * readout[0]
        + jnp.exp(backward_total[None, :] - backward_cum)[..., None] * readout[1]
        + attention_bypass_factor[None, :, None] * x_conv.astype(jnp.float32)
    )
    gated = mixer * jax.nn.silu(result_valve_logits.astype(jnp.float32)).reshape(
        length, heads_here, head_size
    )
    own_sum = jnp.sum(gated * gated, axis=(1, 2))
    if heads_here < spread:
        group_marks = (jnp.arange(GROUPS) == group).astype(jnp.float32)
        group_sums = lax.psum(own_sum[:, None] * group_marks[None, :], "tp")
        own_sum = lax.dynamic_index_in_dim(group_sums, group, 1, keepdims=False)
    scale = lax.rsqrt(own_sum / (spread * HEAD_DIM) + 1e-06)
    normed = (
        gated.reshape(length, channels) * scale[:, None] * cluster_rescale_factor[None, :]
    ).astype(jnp.bfloat16)
    normed_all, rescale_all = gather_tp(
        [normed, specialist_rescale_factor[None, :]], (1, 1), 2
    )
    projected = jnp.dot(normed_all, blender_result_matrix, preferred_element_type=jnp.float32)
    after_mixer = (layer_source_vector.astype(jnp.float32) + projected).astype(jnp.bfloat16)
    resid = after_mixer.astype(jnp.float32)
    (after_all,) = gather_tp([after_mixer], (2,), 3)
    resid_all = after_all.astype(jnp.float32)
    inverse = lax.rsqrt(jnp.sum(resid_all * resid_all, axis=1) / D + 1e-06)[:, None]
    full_features = (resid_all * inverse * rescale_all).astype(jnp.bfloat16)
    features = (resid * inverse * specialist_rescale_factor[None, :]).astype(jnp.bfloat16)
    top = chosen_specialists.shape[1]
    experts = lax.axis_size("sp")
    capacity = 3 * length * top // (2 * experts)
    marks = (
        chosen_specialists[:, :, None] == jnp.arange(experts, dtype=jnp.int32)[None, None, :]
    ).astype(jnp.float32)
    strict = (position[:, None] > position[None, :]).astype(jnp.bfloat16)
    earlier_rows = jnp.dot(
        strict, jnp.sum(marks, axis=1).astype(jnp.bfloat16), preferred_element_type=jnp.float32
    )
    rank = jnp.sum(earlier_rows[:, None, :] * marks, axis=2).astype(jnp.int32)
    slot = chosen_specialists * capacity + rank
    slots = jnp.arange(experts * capacity, dtype=jnp.int32)
    pick = sum((slots[:, None] == slot[None, :, j]).astype(jnp.bfloat16) for j in range(top))
    outgoing = jnp.dot(pick, features, preferred_element_type=jnp.float32).astype(jnp.bfloat16)
    arrived = dispatch(outgoing.reshape(experts, capacity, -1), 4)
    arrived = arrived.reshape(experts * capacity, -1)
    shared_hidden = (
        jax.nn.silu(jnp.dot(full_features, common_valve_matrix, preferred_element_type=jnp.float32))
        * jnp.dot(full_features, common_raising_matrix, preferred_element_type=jnp.float32)
    ).astype(jnp.bfloat16)
    expert_hidden = (
        jax.nn.silu(
            jnp.dot(arrived, specialist_valve_matrix[0], preferred_element_type=jnp.float32)
        )
        * jnp.dot(arrived, specialist_raising_matrix[0], preferred_element_type=jnp.float32)
    ).astype(jnp.bfloat16)
    expert_all, shared_all = gather_tp([expert_hidden, shared_hidden], (4, 2), 5)
    expert_out = jnp.dot(
        expert_all, specialist_lowering_matrix[0], preferred_element_type=jnp.float32
    ).astype(jnp.bfloat16)
    shared_out = jnp.dot(
        shared_all, common_lowering_matrix, preferred_element_type=jnp.float32
    ).astype(jnp.bfloat16)
    (returned,) = swap_sp([expert_out.reshape(experts, capacity, -1)], 6)
    returned = returned.reshape(experts * capacity, -1)
    shares = sum(
        jnp.where(slots[None, :] == slot[:, j, None], specialist_shares[:, j, None], 0.0)
        for j in range(top)
    )
    high = shares.astype(jnp.bfloat16)
    low = (shares - high.astype(jnp.float32)).astype(jnp.bfloat16)
    routed = jnp.dot(high, returned, preferred_element_type=jnp.float32) + jnp.dot(
        low, returned, preferred_element_type=jnp.float32
    )
    return (resid + shared_out.astype(jnp.float32) + routed).astype(jnp.bfloat16)


def solution(mesh):
    return jax.shard_map(
        shards,
        mesh=mesh,
        in_specs=(
            P("sp", "tp"),
            P("sp", "tp"),
            P("sp", "tp"),
            P("sp", None),
            P("sp", None),
            P(None, "sp", "tp"),
            P(None, "tp"),
            P(None, "tp"),
            P(None, "sp", "tp"),
            P("tp"),
            P(None, "tp"),
            P(),
            P(),
            P("tp"),
            P(None, "tp"),
            P("tp"),
            P("sp", None),
            P("sp", None),
            P("sp", None, "tp"),
            P("sp", None, "tp"),
            P("sp", None, "tp"),
            P(None, "tp"),
            P(None, "tp"),
            P(None, "tp"),
        ),
        out_specs=P("sp", "tp"),
        check_vma=False,
    )
```

```python
import functools

import jax
import jax.numpy as jnp
from jax import lax
from jax.experimental import pallas as pl
from jax.experimental.pallas import tpu as pltpu
from jax.sharding import PartitionSpec as P

MESH = pl.DeviceIdType.MESH
KERNEL_DEVICES = 32

D = 2048
HEADS = 16
HEAD_DIM = 64
GROUPS = 4
STATE = 128
CONV = 5


def extended(cells, sides, width):
    for axis, dim in sides:
        count = lax.axis_size(axis)
        ends = count - 1
        head = lax.slice_in_dim(cells, 0, width, axis=dim)
        tail = lax.slice_in_dim(cells, cells.shape[dim] - width, cells.shape[dim], axis=dim)
        cells = jnp.concatenate(
            [
                lax.ppermute(tail, axis, [(i, (i + 1) % count) for i in range(ends)]),
                cells,
                lax.ppermute(head, axis, [((i + 1) % count, i) for i in range(ends)]),
            ],
            axis=dim,
        )
    return cells


def small_mesh():
    return lax.axis_size("sp") * lax.axis_size("tp") <= KERNEL_DEVICES


def greet(axis, peers):
    barrier = pltpu.get_barrier_semaphore()
    for a, peer in zip(axis, peers):
        pl.semaphore_signal(barrier, inc=1, device_id={a: peer}, device_id_type=MESH)
    pl.semaphore_wait(barrier, len(peers))


def remote(src, dst, send, recv, axis, peer):
    return pltpu.make_async_remote_copy(
        src_ref=src,
        dst_ref=dst,
        send_sem=send,
        recv_sem=recv,
        device_id={axis: peer},
        device_id_type=MESH,
    )


def gather_kernel(n, counts, *refs):
    m = len(counts)
    ins, outs = refs[:m], refs[m : 2 * m]
    send_sem, recv_sem, local_sem = refs[2 * m :]
    half = n // 2
    me = lax.axis_index("tp")
    row, core = me // 2, me % 2
    sibling = row * 2 + 1 - core
    onward = [((row + k) % half) * 2 + core for k in range(1, half)]
    origin = [((row + half - k) % half) * 2 + core for k in range(1, half)]
    theirs = [((row + half - k) % half) * 2 + 1 - core for k in range(1, half)]
    greet(["tp"] * half, [sibling] + onward)
    pieces = []
    for i, count in enumerate(counts):
        size = ins[i].shape[0] // count
        for c in range(count):
            pieces.append((i, c * size, size))

    def spot(i, start, size, who):
        width = ins[i].shape[1]
        return outs[i].at[
            pl.ds(start, size), pl.ds(pl.multiple_of(who * width, 128), width)
        ]

    started = []
    for p, (i, start, size) in enumerate(pieces):
        src = ins[i].at[pl.ds(start, size)]
        for k in range(half - 1):
            cp = remote(
                src, spot(i, start, size, me), send_sem.at[1 + k, p], recv_sem.at[1 + k, p], "tp", onward[k]
            )
            cp.start()
            started.append(cp)
    for p, (i, start, size) in enumerate(pieces):
        src = ins[i].at[pl.ds(start, size)]
        cp = remote(src, spot(i, start, size, me), send_sem.at[0, p], recv_sem.at[0, p], "tp", sibling)
        cp.start()
        started.append(cp)
    locals_ = []
    for i in range(m):
        cp = pltpu.make_async_copy(ins[i], spot(i, 0, ins[i].shape[0], me), local_sem.at[i])
        cp.start()
        locals_.append(cp)
    for p, (i, start, size) in enumerate(pieces):
        for k in range(half - 1):
            here = spot(i, start, size, origin[k])
            remote(here, here, send_sem.at[1 + k, p], recv_sem.at[1 + k, p], "tp", sibling).wait_recv()
            cp = remote(here, here, send_sem.at[half + k, p], recv_sem.at[half + k, p], "tp", sibling)
            cp.start()
            started.append(cp)
    for p, (i, start, size) in enumerate(pieces):
        here = spot(i, start, size, sibling)
        remote(here, here, send_sem.at[0, p], recv_sem.at[0, p], "tp", sibling).wait_recv()
        for k in range(half - 1):
            here = spot(i, start, size, theirs[k])
            remote(here, here, send_sem.at[half + k, p], recv_sem.at[half + k, p], "tp", sibling).wait_recv()
    for cp in started:
        cp.wait_send()
    for cp in locals_:
        cp.wait()


def gather_tp(arrays, counts, ident):
    n = lax.axis_size("tp")
    if not small_mesh():
        return [lax.all_gather(a, "tp", axis=1, tiled=True) for a in arrays]
    total = sum(counts)
    return pl.pallas_call(
        functools.partial(gather_kernel, n, counts),
        out_shape=[jax.ShapeDtypeStruct((a.shape[0], a.shape[1] * n), a.dtype) for a in arrays],
        in_specs=[pl.BlockSpec(memory_space=pltpu.VMEM)] * len(arrays),
        out_specs=[pl.BlockSpec(memory_space=pl.ANY)] * len(arrays),
        scratch_shapes=[
            pltpu.SemaphoreType.DMA((n, total)),
            pltpu.SemaphoreType.DMA((n, total)),
            pltpu.SemaphoreType.DMA((len(arrays),)),
        ],
        compiler_params=pltpu.CompilerParams(collective_id=ident, has_side_effects=True),
        name="gather_tp_%d" % ident,
    )(*arrays)


def swap_kernel(n, select, m, *refs):
    ins, outs = refs[:m], refs[m : 2 * m]
    send_sem, recv_sem, local_sem = refs[2 * m :]
    me = lax.axis_index("sp")
    peers = [(me + k) % n for k in range(1, n)]
    greet(["sp"] * (n - 1), peers)
    started = []
    for k in sorted(range(1, n), key=lambda v: -min(v, n - v)):
        for i in range(m):
            row = (me + k) // n if select else peers[k - 1]
            cp = remote(
                ins[i].at[row], outs[i].at[me], send_sem.at[i, k], recv_sem.at[i, k], "sp", peers[k - 1]
            )
            cp.start()
            started.append(cp)
    locals_ = []
    for i in range(m):
        cp = pltpu.make_async_copy(ins[i].at[0 if select else me], outs[i].at[me], local_sem.at[i])
        cp.start()
        locals_.append(cp)
    for k in range(1, n):
        for i in range(m):
            here = outs[i].at[(me + n - k) % n]
            remote(here, here, send_sem.at[i, k], recv_sem.at[i, k], "sp", peers[k - 1]).wait_recv()
    for cp in started:
        cp.wait_send()
    for cp in locals_:
        cp.wait()


def swap_sp(arrays, ident, select=False):
    n = lax.axis_size("sp")
    if not small_mesh():
        if select:
            later = jnp.arange(n) > lax.axis_index("sp")
            arrays = [
                jnp.where(later[:, None, None], a[0][None], a[1][None]) for a in arrays
            ]
        return [lax.all_to_all(a, "sp", split_axis=0, concat_axis=0, tiled=True) for a in arrays]
    m = len(arrays)
    return pl.pallas_call(
        functools.partial(swap_kernel, n, select, m),
        out_shape=[jax.ShapeDtypeStruct((n,) + a.shape[1:], a.dtype) for a in arrays],
        in_specs=[pl.BlockSpec(memory_space=pltpu.VMEM)] * m,
        out_specs=[pl.BlockSpec(memory_space=pl.ANY)] * m,
        scratch_shapes=[
            pltpu.SemaphoreType.DMA((m, n)),
            pltpu.SemaphoreType.DMA((m, n)),
            pltpu.SemaphoreType.DMA((m,)),
        ],
        compiler_params=pltpu.CompilerParams(collective_id=ident, has_side_effects=True),
        name="swap_sp_%d" % ident,
    )(*arrays)


def dispatch(outgoing):
    arrived = lax.all_to_all(outgoing, "sp", split_axis=0, concat_axis=0, tiled=True)
    return lax.all_gather(arrived, "tp", axis=2, tiled=True)


def experts_kernel(n, t, out_blk, feats, wg_ref, wu_ref, wl_ref, sg_ref, su_ref, sl_ref, ret, sout,
                   arr, hid, hall, shid, sall, eout, wg, wu, wl, sg, su, sl,
                   put_s, put_r, fan_s, fan_r, hid_s, hid_r, go_s, go_r, loc):
    half = t // 2
    me, mine = lax.axis_index("sp"), lax.axis_index("tp")
    row, core = mine // 2, mine % 2
    sibling = row * 2 + 1 - core
    onward = [((row + k) % half) * 2 + core for k in range(1, half)]
    origin = [((row + half - k) % half) * 2 + core for k in range(1, half)]
    theirs = [((row + half - k) % half) * 2 + 1 - core for k in range(1, half)]
    peers = [(me + k) % n for k in range(n)]
    source = [(me + n - k) % n for k in range(n)]
    fetch = [
        pltpu.make_async_copy(a, b, loc.at[i])
        for i, (a, b) in enumerate(
            ((sg_ref, sg), (su_ref, su), (wg_ref, wg), (wu_ref, wu), (wl_ref, wl), (sl_ref, sl))
        )
    ]
    for cp in fetch:
        cp.start()
    greet(["sp"] * (n - 1) + ["tp"] * half, peers[1:] + [sibling] + onward)
    started = []

    def columns(who, width):
        return pl.ds(pl.multiple_of(who * width, 128), width)

    def first(k, who):
        return arr.at[source[k], :, columns(who, out_blk.shape[2])]

    def second(k, who):
        if k == n:
            return sall.at[:, columns(who, shid.shape[1])]
        return hall.at[source[k], :, columns(who, hid.shape[2])]

    def fan(src, spot, ss, rr, k):
        for j in range(half - 1):
            cp = remote(src, spot(k, mine), ss.at[1 + j, k], rr.at[1 + j, k], "tp", onward[j])
            cp.start()
            started.append(cp)
        cp = remote(src, spot(k, mine), ss.at[0, k], rr.at[0, k], "tp", sibling)
        cp.start()
        started.append(cp)

    def hand(spot, ss, rr, k):
        for j in range(half - 1):
            here = spot(k, origin[j])
            remote(here, here, ss.at[1 + j, k], rr.at[1 + j, k], "tp", sibling).wait_recv()
            cp = remote(here, here, ss.at[half + j, k], rr.at[half + j, k], "tp", sibling)
            cp.start()
            started.append(cp)

    def landed(spot, ss, rr, k):
        here = spot(k, sibling)
        remote(here, here, ss.at[0, k], rr.at[0, k], "tp", sibling).wait_recv()
        for j in range(half - 1):
            here = spot(k, theirs[j])
            remote(here, here, ss.at[half + j, k], rr.at[half + j, k], "tp", sibling).wait_recv()

    def product(rows, gate, up):
        g = jnp.dot(rows, gate[...], preferred_element_type=jnp.float32)
        return (jax.nn.silu(g) * jnp.dot(rows, up[...], preferred_element_type=jnp.float32)).astype(
            jnp.bfloat16
        )

    far = sorted(range(1, n), key=lambda v: min(v, n - v))
    order = [0] + far
    for k in far:
        cp = remote(out_blk.at[peers[k]], arr.at[me, :, columns(mine, out_blk.shape[2])],
                    put_s.at[k], put_r.at[k], "sp", peers[k])
        cp.start()
        started.append(cp)
    keep = pltpu.make_async_copy(out_blk.at[me], first(0, mine), loc.at[6])
    keep.start()
    locals_ = [keep]

    def arrive(k):
        if k == 0:
            fan(out_blk.at[me], first, fan_s, fan_r, 0)
            return
        here = first(k, mine)
        remote(here, here, put_s.at[k], put_r.at[k], "sp", peers[k]).wait_recv()
        fan(here, first, fan_s, fan_r, k)

    def spread(k):
        src = shid if k == n else hid.at[source[k]]
        fan(src, second, hid_s, hid_r, k)
        cp = pltpu.make_async_copy(src, second(k, mine), loc.at[7 + k])
        cp.start()
        locals_.append(cp)
        return cp

    own = {}

    def hidden(k):
        landed(first, fan_s, fan_r, k)
        if k == 0:
            keep.wait()
            fetch[2].wait()
            fetch[3].wait()
        hid[source[k]] = product(arr[source[k]], wg, wu)

    def lowering(k):
        landed(second, hid_s, hid_r, k)
        own[k].wait()
        if k == 0:
            fetch[4].wait()
        eout[source[k]] = jnp.dot(
            hall[source[k]], wl[...], preferred_element_type=jnp.float32
        ).astype(eout.dtype)

    def give(k):
        src = eout.at[source[k]]
        if k == 0:
            cp = pltpu.make_async_copy(src, ret.at[me], loc.at[8 + n])
            cp.start()
            own[-1] = cp
            return
        cp = remote(src, ret.at[me], go_s.at[k], go_r.at[k], "sp", source[k])
        cp.start()
        started.append(cp)

    lag = 4
    for s in range(n + lag):
        if s < n:
            arrive(order[s])
        if s == 0:
            fetch[0].wait()
            fetch[1].wait()
            shid[...] = product(feats[...], sg, su)
        if s == 1:
            own[n] = spread(n)
        if 3 <= s <= lag:
            own[order[s - 3]] = spread(order[s - 3])
        if s == 3:
            hand(second, hid_s, hid_r, n)
        if 1 <= s <= n:
            hand(first, fan_s, fan_r, order[s - 1])
        if lag <= s < n + lag:
            hand(second, hid_s, hid_r, order[s - lag])
        if 2 <= s < n + 2:
            hidden(order[s - 2])
        if lag + 1 <= s < n + lag:
            give(order[s - lag - 1])
        if lag <= s < n + lag:
            lowering(order[s - lag])
        if lag <= s < n + 2:
            own[order[s - 2]] = spread(order[s - 2])
    landed(second, hid_s, hid_r, n)
    own[n].wait()
    fetch[5].wait()
    sout[...] = jnp.dot(sall[...], sl[...], preferred_element_type=jnp.float32).astype(sout.dtype)
    give(order[n - 1])
    for k in far:
        here = ret.at[peers[k]]
        remote(here, here, go_s.at[k], go_r.at[k], "sp", source[k]).wait_recv()
    for cp in started:
        cp.wait_send()
    own[-1].wait()


def all_experts(outgoing, features, weights, ident):
    n, t = lax.axis_size("sp"), lax.axis_size("tp")
    blocks, slots, columns = outgoing.shape
    length = features.shape[0]
    units, out = weights[0].shape[1], weights[2].shape[1]
    vmem, anywhere = pl.BlockSpec(memory_space=pltpu.VMEM), pl.BlockSpec(memory_space=pl.ANY)
    half = jnp.bfloat16
    return pl.pallas_call(
        functools.partial(experts_kernel, n, t),
        out_shape=[
            jax.ShapeDtypeStruct((blocks, slots, out), half),
            jax.ShapeDtypeStruct((length, out), half),
        ],
        in_specs=[vmem, vmem] + [anywhere] * 6,
        out_specs=[anywhere, vmem],
        scratch_shapes=[
            pltpu.VMEM((blocks, slots, columns * t), half),
            pltpu.VMEM((blocks, slots, units), half),
            pltpu.VMEM((blocks, slots, units * t), half),
            pltpu.VMEM((length, units), half),
            pltpu.VMEM((length, units * t), half),
            pltpu.VMEM((blocks, slots, out), half),
        ]
        + [pltpu.VMEM(w.shape, half) for w in weights]
        + [
            pltpu.SemaphoreType.DMA((n,)),
            pltpu.SemaphoreType.DMA((n,)),
            pltpu.SemaphoreType.DMA((t, n)),
            pltpu.SemaphoreType.DMA((t, n)),
            pltpu.SemaphoreType.DMA((t, n + 1)),
            pltpu.SemaphoreType.DMA((t, n + 1)),
            pltpu.SemaphoreType.DMA((n,)),
            pltpu.SemaphoreType.DMA((n,)),
            pltpu.SemaphoreType.DMA((n + 9,)),
        ],
        compiler_params=pltpu.CompilerParams(
            collective_id=ident, has_side_effects=True, vmem_limit_bytes=48 * 1024 * 1024
        ),
        name="experts_%d" % ident,
    )(outgoing, features, *weights)


def lowered(hidden, shared, weight, shared_weight):
    n, t = lax.axis_size("sp"), lax.axis_size("tp")
    blocks, slots, _ = hidden.shape
    out = weight.shape[1]
    hidden_all, shared_all = gather_tp([hidden.reshape(blocks * slots, -1), shared], (1, 1), 0)
    mine = jnp.dot(hidden_all, weight, preferred_element_type=jnp.float32).astype(jnp.bfloat16)
    (back,) = swap_sp([mine.reshape(blocks, slots, out)], 0)
    return back, jnp.dot(
        shared_all, shared_weight, preferred_element_type=jnp.float32
    ).astype(jnp.bfloat16)


def shards(
    layer_source_vector,
    attention_lane_source,
    result_valve_logits,
    memory_write_matrix,
    memory_query_matrix,
    increment_logits,
    increment_offset,
    log_fade_speed,
    extra_log_fade,
    attention_bypass_factor,
    attention_lane_kernel,
    memory_write_kernel,
    memory_query_kernel,
    cluster_rescale_factor,
    blender_result_matrix,
    specialist_rescale_factor,
    chosen_specialists,
    specialist_shares,
    specialist_valve_matrix,
    specialist_raising_matrix,
    specialist_lowering_matrix,
    common_valve_matrix,
    common_raising_matrix,
    common_lowering_matrix,
):
    length = attention_lane_source.shape[0]
    heads_here = increment_offset.shape[1]
    channels = attention_lane_source.shape[1]
    head_size = channels // heads_here
    spread = HEADS // GROUPS
    group = lax.axis_index("tp") * heads_here // spread
    b_own = lax.dynamic_slice_in_dim(memory_write_matrix, group * STATE, STATE, 1)
    c_own = lax.dynamic_slice_in_dim(memory_query_matrix, group * STATE, STATE, 1)
    joined = jnp.concatenate([attention_lane_source, b_own, c_own], axis=1)
    taps = jnp.concatenate(
        [
            attention_lane_kernel,
            lax.dynamic_slice_in_dim(memory_write_kernel, group * STATE, STATE, 1),
            lax.dynamic_slice_in_dim(memory_query_kernel, group * STATE, STATE, 1),
        ],
        axis=1,
    )
    padded = extended(joined, (("sp", 0),), CONV // 2)
    total = jnp.zeros(joined.shape, jnp.float32)
    for offset in range(CONV):
        total = total + padded[offset : offset + length].astype(jnp.float32) * taps[offset].astype(
            jnp.float32
        )
    convolved = jax.nn.silu(total).astype(jnp.bfloat16)
    x_conv = convolved[:, :channels].reshape(length, heads_here, head_size)
    b_conv = convolved[:, channels : channels + STATE]
    c_conv = convolved[:, channels + STATE :]
    increment_lengths = jax.nn.softplus(
        increment_logits.astype(jnp.float32) + increment_offset[:, None, :]
    )
    log_fade_amount = -jnp.exp(log_fade_speed)[:, None, :] * increment_lengths + extra_log_fade
    position = jnp.arange(length)
    lower = position[:, None] >= position[None, :]
    upper = position[:, None] <= position[None, :]
    both = jnp.concatenate([log_fade_amount[0], log_fade_amount[1]], axis=1)
    sums = jnp.dot(
        lower.astype(jnp.float32),
        both,
        precision=lax.Precision.HIGHEST,
        preferred_element_type=jnp.float32,
    )
    forward_cum = sums[:, :heads_here]
    backward_cum = sums[:, heads_here:] - log_fade_amount[1]
    forward_total = sums[-1, :heads_here]
    backward_total = sums[-1, heads_here:]
    scores = lax.dot_general(
        c_conv, b_conv, (((1,), (1,)), ((), ())), preferred_element_type=jnp.float32
    )
    forward_gap = forward_cum.T[:, :, None] - forward_cum.T[:, None, :]
    backward_gap = backward_cum.T[:, None, :] - backward_cum.T[:, :, None]
    forward_part = (
        jnp.where(lower, jnp.exp(jnp.where(lower, forward_gap, 0.0)), 0.0)
        * increment_lengths[0].T[:, None, :]
    )
    backward_part = (
        jnp.where(upper, jnp.exp(jnp.where(upper, backward_gap, 0.0)), 0.0)
        * increment_lengths[1].T[:, None, :]
    )
    mixing = (scores[None] * (forward_part + backward_part)).astype(jnp.bfloat16)
    inner = jnp.einsum("hts,shp->thp", mixing, x_conv, preferred_element_type=jnp.float32)
    forward_scale = jnp.exp(forward_total[None, :] - forward_cum) * increment_lengths[0]
    backward_scale = jnp.exp(backward_cum) * increment_lengths[1]
    scaled = (
        jnp.stack([forward_scale, backward_scale])[..., None] * x_conv.astype(jnp.float32)[None]
    ).astype(jnp.bfloat16)
    own_states = jnp.einsum("dshp,sn->dhpn", scaled, b_conv, preferred_element_type=jnp.float32)
    own_logs = jnp.stack([forward_total, backward_total])
    blocks = lax.axis_size("sp")
    own_index = lax.axis_index("sp")
    states_all, logs_all = swap_sp(
        [
            own_states.astype(jnp.bfloat16).reshape(2, heads_here * head_size, STATE),
            jnp.broadcast_to(own_logs[:, :, None], (2, heads_here, 128)),
        ],
        1,
        True,
    )
    logs_all = logs_all[:, :, 0]
    states_all = states_all.reshape(blocks, heads_here, head_size, STATE).astype(jnp.float32)
    index = jnp.arange(blocks)
    earlier = (index < own_index)[:, None]
    later = (index > own_index)[:, None]
    after = (index[None, :] > index[:, None])[:, :, None]
    ahead = (index[None, :] < index[:, None])[:, :, None]
    gap_forward = jnp.sum(jnp.where(after & earlier[None], logs_all[None], 0.0), axis=1)
    gap_backward = jnp.sum(jnp.where(ahead & later[None], logs_all[None], 0.0), axis=1)
    weight_forward = jnp.where(earlier, jnp.exp(jnp.where(earlier, gap_forward, 0.0)), 0.0)
    weight_backward = jnp.where(later, jnp.exp(jnp.where(later, gap_backward, 0.0)), 0.0)
    weights = jnp.stack([weight_forward, weight_backward])
    carried = jnp.sum(weights[:, :, :, None, None] * states_all[None], axis=1).astype(jnp.bfloat16)
    readout = jnp.einsum("tn,dhpn->dthp", c_conv, carried, preferred_element_type=jnp.float32)
    mixer = (
        inner
        + jnp.exp(forward_cum)[..., None] * readout[0]
        + jnp.exp(backward_total[None, :] - backward_cum)[..., None] * readout[1]
        + attention_bypass_factor[None, :, None] * x_conv.astype(jnp.float32)
    )
    gated = mixer * jax.nn.silu(result_valve_logits.astype(jnp.float32)).reshape(
        length, heads_here, head_size
    )
    own_sum = jnp.sum(gated * gated, axis=(1, 2))
    if heads_here < spread:
        group_marks = (jnp.arange(GROUPS) == group).astype(jnp.float32)
        group_sums = lax.psum(own_sum[:, None] * group_marks[None, :], "tp")
        own_sum = lax.dynamic_index_in_dim(group_sums, group, 1, keepdims=False)
    scale = lax.rsqrt(own_sum / (spread * HEAD_DIM) + 1e-06)
    normed = (
        gated.reshape(length, channels) * scale[:, None] * cluster_rescale_factor[None, :]
    ).astype(jnp.bfloat16)
    normed_all, rescale_all = gather_tp(
        [normed, specialist_rescale_factor[None, :]], (1, 1), 2
    )
    projected = jnp.dot(normed_all, blender_result_matrix, preferred_element_type=jnp.float32)
    after_mixer = (layer_source_vector.astype(jnp.float32) + projected).astype(jnp.bfloat16)
    resid = after_mixer.astype(jnp.float32)
    (after_all,) = gather_tp([after_mixer], (2,), 3)
    resid_all = after_all.astype(jnp.float32)
    inverse = lax.rsqrt(jnp.sum(resid_all * resid_all, axis=1) / D + 1e-06)[:, None]
    full_features = (resid_all * inverse * rescale_all).astype(jnp.bfloat16)
    features = (resid * inverse * specialist_rescale_factor[None, :]).astype(jnp.bfloat16)
    top = chosen_specialists.shape[1]
    experts = lax.axis_size("sp")
    capacity = 3 * length * top // (2 * experts)
    marks = (
        chosen_specialists[:, :, None] == jnp.arange(experts, dtype=jnp.int32)[None, None, :]
    ).astype(jnp.float32)
    strict = (position[:, None] > position[None, :]).astype(jnp.bfloat16)
    earlier_rows = jnp.dot(
        strict, jnp.sum(marks, axis=1).astype(jnp.bfloat16), preferred_element_type=jnp.float32
    )
    rank = jnp.sum(earlier_rows[:, None, :] * marks, axis=2).astype(jnp.int32)
    slot = chosen_specialists * capacity + rank
    slots = jnp.arange(experts * capacity, dtype=jnp.int32)
    pick = sum((slots[:, None] == slot[None, :, j]).astype(jnp.bfloat16) for j in range(top))
    outgoing = jnp.dot(pick, features, preferred_element_type=jnp.float32).astype(jnp.bfloat16)
    outgoing = outgoing.reshape(experts, capacity, -1)
    products = (
        specialist_valve_matrix[0],
        specialist_raising_matrix[0],
        specialist_lowering_matrix[0],
        common_valve_matrix,
        common_raising_matrix,
        common_lowering_matrix,
    )
    if small_mesh():
        returned, shared_out = all_experts(outgoing, full_features, products, 4)
    else:
        arrived = dispatch(outgoing).reshape(experts * capacity, -1)
        gate, up, down, shared_gate, shared_up, shared_down = products

        def hidden_of(rows, one, two):
            return (
                jax.nn.silu(jnp.dot(rows, one, preferred_element_type=jnp.float32))
                * jnp.dot(rows, two, preferred_element_type=jnp.float32)
            ).astype(jnp.bfloat16)

        returned, shared_out = lowered(
            hidden_of(arrived, gate, up).reshape(experts, capacity, -1),
            hidden_of(full_features, shared_gate, shared_up),
            down,
            shared_down,
        )
    returned = returned.reshape(experts * capacity, -1)
    shares = sum(
        jnp.where(slots[None, :] == slot[:, j, None], specialist_shares[:, j, None], 0.0)
        for j in range(top)
    )
    high = shares.astype(jnp.bfloat16)
    low = (shares - high.astype(jnp.float32)).astype(jnp.bfloat16)
    routed = jnp.dot(high, returned, preferred_element_type=jnp.float32) + jnp.dot(
        low, returned, preferred_element_type=jnp.float32
    )
    return (resid + shared_out.astype(jnp.float32) + routed).astype(jnp.bfloat16)


def solution(mesh):
    return jax.shard_map(
        shards,
        mesh=mesh,
        in_specs=(
            P("sp", "tp"),
            P("sp", "tp"),
            P("sp", "tp"),
            P("sp", None),
            P("sp", None),
            P(None, "sp", "tp"),
            P(None, "tp"),
            P(None, "tp"),
            P(None, "sp", "tp"),
            P("tp"),
            P(None, "tp"),
            P(),
            P(),
            P("tp"),
            P(None, "tp"),
            P("tp"),
            P("sp", None),
            P("sp", None),
            P("sp", None, "tp"),
            P("sp", None, "tp"),
            P("sp", None, "tp"),
            P(None, "tp"),
            P(None, "tp"),
            P(None, "tp"),
        ),
        out_specs=P("sp", "tp"),
        check_vma=False,
    )
```
